32 devices in a mesh: grp: 2 (over y), ep: 8 (over z, core), tp: 2 (over x).
Axes of the slice: x: 2, y: 2, z: 4, core: 2. Of those that a mesh axis runs over, the one named last changes fastest.
Arguments:
- tokens: bfloat16 [512, 2048], P(('grp', 'ep')), parts along dimension 0, may hold values from -12 to 12
- routes: int32 [512, 4], P(('grp', 'ep')), parts along dimension 0, may hold values from 0 to 7, all different within a row; in each aligned block of 32 rows (0 to 31, 32 to 63, ...) at most 32 rows name the same one
- gates: float32 [512, 4], P(('grp', 'ep')), parts along dimension 0, may hold values from 0.1 to 1
- norm_gain: bfloat16 [2048], replicated, may hold values from 0.099609375 to 1.8984375
- exp_gate: bfloat16 [8, 2048, 2048], P('ep', None, 'tp'), may hold values from -0.125 to 0.125
- exp_up: bfloat16 [8, 2048, 2048], P('ep', None, 'tp'), may hold values from -0.125 to 0.125
- exp_down: bfloat16 [8, 2048, 2048], P('ep', 'tp'), may hold values from -0.26516504 to 0.26516504
- sh_gate: bfloat16 [2048, 1024], P(None, 'tp'), may hold values from -0.125 to 0.125
- sh_up: bfloat16 [2048, 1024], P(None, 'tp'), may hold values from -0.125 to 0.125
- sh_down: bfloat16 [1024, 2048], P('tp'), may hold values from -0.375 to 0.375
- out_gain: bfloat16 [2048], P('tp'), may hold values from 0.099609375 to 1.8984375
Outputs:
- mixed: bfloat16 [512, 2048], P(('grp', 'ep'), 'tp'), parts along dimension 0
The draws below stay inside these ranges and needn't reach their ends.
There are 2 independent parts, one for each index of `grp`. The reference program is written for one: setup_inputs(seed, part) draws one part's arguments, and reference() takes and returns one part's arrays. A program takes and returns all parts, laid end to end along the dimension named above; an argument that names none is the same for every part. Nothing has to cross between parts.
Inputs may be any that keep to these rules, and one draw needn't show every extreme that they name: `routes`: each row names 4 different experts; within the rows of one device (aligned blocks of 32 rows) no expert is named by more than 32 rows, a bound that some block reaches.
All inputs are finite; a program needn't handle non-finite values.
Results may differ from the reference program's by a relative error of at most 0.015.
Values may be sent and summed in bfloat16 or wider, within the bound.
No kernel may reach another device: no remote copies, remote signals or barrier semaphores. Data moves between devices by JAX's collectives and lax.ppermute only.
A program may use at most 64 MiB of HBM per device.

```python
import math
import jax
import jax.numpy as jnp
import numpy as np
from jax import lax

D = 2048
FF = 2048
SHARED_FF = 1024
TOP_K = 4
TOK_EP = 32
EXPERTS = 8
TOKENS = 256
CAP = 32
N_EP = 8
N_TP = 2


def rising_down(key, array_shape, fan_in):
    column = jnp.arange(D, dtype=jnp.float32) / (D - 1)
    base_draw = jnp.clip(jax.random.normal(key, array_shape, jnp.float32), -4.0, 4.0)
    profile = 5.0 ** (column - 0.5)
    return (base_draw * profile * fan_in ** (-0.5)).astype(jnp.bfloat16)


def draw_exp_down(key, part):
    return rising_down(jax.random.fold_in(key, 11), (EXPERTS, FF, D), FF)


def draw_sh_down(key, part):
    return rising_down(jax.random.fold_in(key, 23), (SHARED_FF, D), SHARED_FF)


def shard_levels(own_key, extent, cuts, least, top_value):
    def one(dim, blocks):
        heights = jax.random.uniform(jax.random.fold_in(jax.random.fold_in(own_key, 6), dim), (blocks,), jnp.float32, least / len(cuts), top_value / len(cuts))
        return jnp.repeat(jnp.exp(heights), extent[dim] // blocks).reshape((-1,) + (1,) * (len(extent) - dim - 1))

    factor_of = one(*cuts[0])
    for cut in cuts[1:]:
        factor_of = factor_of * one(*cut)
    return factor_of


def shared_out(rng, own, number, rows, amount, top, most, skew):
    ranking = jax.random.permutation(rng, amount)
    packed, usual = load_shares(amount, rows * top, most, skew, True), load_shares(amount, rows * top, most, skew, False)
    places = jnp.arange(amount)

    def named(sizes, rotation):
        used = int((sizes > 0).sum())
        fixed = max(1, used // 4)
        moved = fixed + (places - fixed + rotation * (used - fixed)) % max(1, amount - fixed)
        return jnp.zeros((amount,), jnp.int32).at[ranking[jnp.where(places < fixed, places, moved)]].set(jnp.asarray(sizes, jnp.int32))

    sizes = jnp.where(number % 4 == 0, named(packed, number // 4), named(usual, number - number // 4 - 1))
    mixed = jax.random.permutation(jax.random.fold_in(own, 3), amount)
    giver, receiver = mixed[0:amount // 2 * 2:2], mixed[1:amount // 2 * 2:2]
    margin = jnp.minimum(sizes[giver] - 1, most - sizes[receiver]) // 2
    margin = jnp.where((giver == ranking[0]) | (receiver == ranking[0]) | (sizes[receiver] == 0), 0, jnp.maximum(margin, 0))
    moved = jax.random.randint(jax.random.fold_in(own, 4), (amount // 2,), 0, 1 << 20) % (margin + 1)
    sizes = sizes.at[giver].add(-moved).at[receiver].add(moved)
    labels = jnp.searchsorted(jnp.cumsum(sizes), jnp.arange(rows * top), side="right").astype(jnp.int32)
    listing = labels.reshape(top, rows).T
    listing = listing[jax.random.permutation(jax.random.fold_in(own, 1), rows)]
    rotation = jax.random.randint(jax.random.fold_in(own, 2), (rows, 1), 0, top)
    return jnp.take_along_axis(listing, (jnp.arange(top)[None, :] + rotation) % top, axis=1)


def load_shares(count, total, reach, slope, full):
    portions = [(1 << 20) // math.isqrt(standing ** slope) + 1 for standing in range(1, count + 1)]
    largest = reach if full else min(reach, max(-(-total // count), total * portions[0] // sum(portions)))
    least = 1 if total - largest >= count - 1 else 0
    given, surplus = [largest] + [least] * (count - 1), total - largest - least * (count - 1)
    while surplus > 0:
        movable = [i for i in range(1, count) if given[i] < largest] or [i for i in range(1, count) if given[i] < reach]
        pool, budget = sum([portions[i] for i in movable]), surplus
        for i in movable:
            extra = min(reach - given[i], max(1, budget * portions[i] // pool), surplus)
            given[i] = given[i] + extra
            surplus = surplus - extra
    return np.array(given)


def normal_values(stream_key, dims, scale, reach, cuts=(), held_as=jnp.bfloat16):
    result = jax.random.normal(stream_key, dims, jnp.float32) * scale
    if len(cuts) > 0:
        result = shard_levels(stream_key, dims, cuts, -0.22, 0.18) * result
    return jnp.clip(result, min=-reach, max=reach).astype(held_as)


def setup_inputs(seed: int = 0, part: int = 0) -> dict:
    seeds = jax.random.split(jax.random.key(seed), 12)
    part_keys = jax.random.split(jax.random.fold_in(seeds[11], part), 12)
    tokens = normal_values(part_keys[0], (TOKENS, D), 2.0, 12.0, ((0, 8),))
    routes_keys = jax.random.split(jax.random.fold_in(part_keys[1], 1), TOKENS // TOK_EP)
    routes_turns = jax.random.permutation(jax.random.fold_in(part_keys[1], 3), TOKENS // TOK_EP)
    routes = jax.vmap(lambda own, number: shared_out(jax.random.fold_in(part_keys[1], 2), own, number, TOK_EP, EXPERTS, TOP_K, CAP, 2))(routes_keys, routes_turns).reshape((TOKENS, TOP_K))
    gates = jnp.clip(jnp.exp(math.log(1.0) - 2.3025851 * jax.random.uniform(part_keys[2], (TOKENS, TOP_K), jnp.float32) ** shard_levels(part_keys[2], (TOKENS, TOP_K), ((0, 8),), -0.2, 0.2)), 0.1, 1.0)
    norm_gain = jnp.clip(1.0 + 0.18 * jax.random.normal(seeds[3], (D,), jnp.float32), 0.099609375, 1.8984375).astype(jnp.bfloat16)
    exp_gate = normal_values(seeds[4], (EXPERTS, D, FF), D ** -0.5, 0.125, ((0, 8), (2, 2)))
    exp_up = normal_values(seeds[5], (EXPERTS, D, FF), D ** -0.5, 0.125, ((0, 8), (2, 2)))
    exp_down = draw_exp_down(jax.random.fold_in(seeds[11], 71), part)
    sh_gate = normal_values(seeds[7], (D, SHARED_FF), D ** -0.5, 0.125, ((1, 2),))
    sh_up = normal_values(seeds[8], (D, SHARED_FF), D ** -0.5, 0.125, ((1, 2),))
    sh_down = draw_sh_down(jax.random.fold_in(seeds[11], 71), part)
    out_gain = jnp.clip(1.0 + 0.18 * jax.random.normal(seeds[10], (D,), jnp.float32), 0.099609375, 1.8984375).astype(jnp.bfloat16)
    return {"tokens": tokens, "routes": routes, "gates": gates, "norm_gain": norm_gain, "exp_gate": exp_gate, "exp_up": exp_up, "exp_down": exp_down, "sh_gate": sh_gate, "sh_up": sh_up, "sh_down": sh_down, "out_gain": out_gain}


EPSILON = 1e-06

def slot_order(flat_routes, count):
    hits = (flat_routes[:, None] == jnp.arange(count, dtype=jnp.int32)[None, :]).astype(jnp.int32)
    before = jnp.cumsum(hits, axis=0) - hits
    return lax.optimization_barrier(jnp.sum(before * hits, axis=1)).astype(jnp.int32)

def swiglu_blocks(row_block, w_gate, w_up, w_down):
    gate_act = jnp.dot(row_block, w_gate, preferred_element_type=jnp.float32)
    up_act = jnp.dot(row_block, w_up, preferred_element_type=jnp.float32)
    hidden = (jax.nn.silu(gate_act) * up_act).astype(jnp.bfloat16)
    width = w_down.shape[0] // N_TP
    pieces = jnp.einsum('rnf,nfd->nrd', hidden.astype(jnp.float32).reshape(row_block.shape[0], N_TP, width), w_down.astype(jnp.float32).reshape(N_TP, width, w_down.shape[1]))
    rounded = lax.optimization_barrier(pieces.astype(jnp.bfloat16)).astype(jnp.float32)
    return lax.optimization_barrier(jnp.sum(rounded, axis=0)).astype(jnp.bfloat16)

def reference(tokens, routes, gates, norm_gain, exp_gate, exp_up, exp_down, sh_gate, sh_up, sh_down, out_gain):
    values = tokens.astype(jnp.float32)
    normed = (values * lax.rsqrt(lax.optimization_barrier(jnp.mean(values * values, axis=1, keepdims=True)) + EPSILON) * norm_gain.astype(jnp.float32)).astype(jnp.bfloat16)
    flat_expert = routes.reshape(-1).astype(jnp.int32)
    slot_index = jax.vmap(lambda block_routes: slot_order(block_routes, EXPERTS))(routes.reshape(N_EP, TOK_EP * TOP_K).astype(jnp.int32)).reshape(-1)
    flat_token = jnp.repeat(jnp.arange(TOKENS, dtype=jnp.int32), TOP_K)
    source = flat_token // TOK_EP
    position = flat_expert * (N_EP * CAP) + source * CAP + slot_index
    token_table = jnp.zeros((EXPERTS * N_EP * CAP,), jnp.int32).at[position].set(flat_token)
    weight_table = jnp.zeros((EXPERTS * N_EP * CAP,), jnp.float32).at[position].set(gates.reshape(-1))

    def one_expert(inputs):
        token_index, w_gate, w_up, w_down = inputs
        return swiglu_blocks(normed[token_index], w_gate, w_up, w_down)
    outputs = lax.map(one_expert, (token_table.reshape(EXPERTS, N_EP * CAP), exp_gate, exp_up, exp_down))
    routed = jnp.zeros((TOKENS, D), jnp.float32).at[token_table].add(weight_table[:, None] * outputs.reshape(-1, D).astype(jnp.float32))
    shared = swiglu_blocks(normed, sh_gate, sh_up, sh_down).astype(jnp.float32)
    total = routed + shared
    scale = lax.rsqrt(lax.optimization_barrier(jnp.mean(total * total, axis=1, keepdims=True)) + EPSILON)
    return (total * scale * out_gain.astype(jnp.float32)).astype(jnp.bfloat16)
```

```python
import jax
import jax.numpy as jnp
from jax import lax
from jax.sharding import PartitionSpec as P

EPSILON = 1e-06
LANES = 128


def shards(
    tokens, routes, gates, norm_gain, exp_gate, exp_up, exp_down, sh_gate, sh_up, sh_down, out_gain
):
    ep = lax.axis_size("ep")
    tp = lax.axis_size("tp")
    assert tp & (tp - 1) == 0 and ep & (ep - 1) == 0 and exp_gate.shape[0] == 1
    rows, width = tokens.shape
    half = width // tp
    chips = ep // 2
    me = lax.axis_index("ep")
    side = lax.axis_index("tp")
    f32, bf16 = jnp.float32, jnp.bfloat16

    def across(x, bits):
        return lax.ppermute(x, "ep", [(i, i ^ bits) for i in range(ep)])

    def over_tp(x, bits):
        return lax.ppermute(x, "tp", [(i, i ^ bits) for i in range(tp)])

    def features(x, index):
        if tp == 2:
            return jnp.where(index == 0, x[..., :half], x[..., half:])
        return lax.dynamic_slice_in_dim(x, index * half, half, axis=x.ndim - 1)

    values = tokens.astype(f32)
    normed = (
        values
        * lax.rsqrt(jnp.mean(values * values, axis=1, keepdims=True) + EPSILON)
        * norm_gain.astype(f32)
    ).astype(bf16)
    extra = (2 * ep + LANES - 1) // LANES * LANES
    column = jnp.arange(extra, dtype=jnp.int32)
    weight = jnp.sum(
        jnp.where(routes[:, :, None] == (column % ep)[None, None, :], gates[:, :, None], 0.0), axis=1
    )
    coarse = weight.astype(bf16)
    fine = (weight - coarse.astype(f32)).astype(bf16)
    packed = jnp.where(column < ep, coarse, jnp.where(column < 2 * ep, fine, jnp.zeros((), bf16)))
    block = jnp.concatenate([normed, packed], axis=1)

    mine = [block] + [across(block, 2 * k) for k in range(1, chips)]
    theirs = [across(b, 1) for b in mine]

    shared_gate = jnp.dot(normed, sh_gate, preferred_element_type=f32)
    shared_up = jnp.dot(normed, sh_up, preferred_element_type=f32)
    shared_hidden = (jax.nn.silu(shared_gate) * shared_up).astype(bf16)
    shared_part = jnp.dot(shared_hidden, sh_down, preferred_element_type=f32)

    gathered = jnp.concatenate(theirs + mine, axis=0)
    inputs = gathered[:, :width]
    lanes = gathered[:, width:].astype(f32)
    mix = jnp.sum(jnp.where((column % ep == me)[None, :] & (column < 2 * ep), lanes, 0.0), axis=1)
    gate_act = jnp.dot(inputs, exp_gate[0], preferred_element_type=f32)
    up_act = jnp.dot(inputs, exp_up[0], preferred_element_type=f32)
    hidden = (jax.nn.silu(gate_act) * up_act * mix[:, None]).astype(bf16)
    part = jnp.dot(hidden, exp_down[0], preferred_element_type=f32).astype(bf16)

    other = across(part[: chips * rows], 1)
    paired = part[chips * rows :].astype(f32) + other.astype(f32)
    paired = paired.reshape(chips, rows, width)
    paired = [paired[0] + shared_part] + [paired[k] for k in range(1, chips)]
    arrived = {}
    for k in list(range(1, chips)) + [0]:
        arrived[k] = features(paired[k], side)
        for bits in range(1, tp):
            sent = features(paired[k], side ^ bits).astype(bf16)
            arrived[k] = arrived[k] + over_tp(sent, bits).astype(f32)
    total = arrived[0]
    for k in range(1, chips):
        total = total + across(arrived[k].astype(bf16), 2 * k).astype(f32)
    own_squares = jnp.sum(total * total, axis=1)
    squares = own_squares
    for bits in range(1, tp):
        squares = squares + over_tp(own_squares, bits)
    scale = lax.rsqrt(squares / width + EPSILON)
    return (total * scale[:, None] * out_gain.astype(f32)).astype(bf16)


def solution(mesh):
    placed = (
        P(("grp", "ep"), None),
        P(("grp", "ep"), None),
        P(("grp", "ep"), None),
        P(),
        P("ep", None, "tp"),
        P("ep", None, "tp"),
        P("ep", "tp", None),
        P(None, "tp"),
        P(None, "tp"),
        P("tp", None),
        P("tp"),
    )
    return jax.shard_map(
        shards, mesh=mesh, in_specs=placed, out_specs=P(("grp", "ep"), "tp"), check_vma=False
    )
```

```python
import jax
import jax.numpy as jnp
from jax import lax
from jax.experimental import pallas as pl
from jax.experimental.pallas import tpu as pltpu
from jax.sharding import PartitionSpec as P

EPSILON = 1e-06
LANES = 128


def fetch_body(tie, gate, up, down, gate_out, up_out, down_out, sems):
    copies = [
        pltpu.make_async_copy(gate.at[0], gate_out, sems.at[0]),
        pltpu.make_async_copy(up.at[0], up_out, sems.at[1]),
        pltpu.make_async_copy(down.at[0], down_out, sems.at[2]),
    ]
    for copy in copies:
        copy.start()
    for copy in copies:
        copy.wait()


def fetch(tie, gate, up, down):
    hbm = pl.BlockSpec(memory_space=pltpu.HBM)
    gate, up, down = [pltpu.with_memory_space_constraint(w, pltpu.HBM) for w in (gate, up, down)]
    vmem = pl.BlockSpec(memory_space=pltpu.VMEM)
    return pl.pallas_call(
        fetch_body,
        in_specs=[vmem, hbm, hbm, hbm],
        out_specs=[vmem, vmem, vmem],
        out_shape=[pltpu.VMEM(w.shape[1:], w.dtype) for w in (gate, up, down)],
        scratch_shapes=[pltpu.SemaphoreType.DMA((3,))],
        cost_estimate=pl.CostEstimate(
            flops=4 * 10**9, transcendentals=0, bytes_accessed=2 * (gate.size + up.size + down.size)
        ),
        compiler_params=pltpu.CompilerParams(vmem_limit_bytes=2 << 20),
        name="fetch_weights",
    )(tie, gate, up, down)


def expert_body(count, *refs):
    blocks = refs[:count]
    place, gate, up, down, away, home, tokens, hidden = refs[count:]
    rows = blocks[0].shape[0]
    width = gate.shape[0]
    ff = gate.shape[1]
    step = min(256, ff)
    for i in range(count):
        tokens[i * rows : (i + 1) * rows, :] = blocks[i][...]
    lanes = tokens[:, width:].astype(jnp.float32)
    mix = jnp.sum(lanes * place[...], axis=1, keepdims=True)
    x = tokens[:, :width]
    for j in range(ff // step):
        cut = slice(j * step, (j + 1) * step)
        g = jnp.dot(x, gate[:, cut], preferred_element_type=jnp.float32)
        u = jnp.dot(x, up[:, cut], preferred_element_type=jnp.float32)
        hidden[:, cut] = (g / (1.0 + jnp.exp(-g)) * u * mix).astype(jnp.bfloat16)
    cutoff = away.shape[0]
    span = min(512, width)
    for j in range(width // span):
        cut = slice(j * span, (j + 1) * span)
        out = jnp.dot(hidden[...], down[:, cut], preferred_element_type=jnp.float32)
        away[:, cut] = out[:cutoff].astype(jnp.bfloat16)
        home[:, cut] = out[cutoff:]


def expert(blocks, place, gate, up, down):
    count = len(blocks)
    rows, wide = blocks[0].shape
    all_rows = count * rows
    gate, up, down = [pltpu.with_memory_space_constraint(w, pltpu.VMEM) for w in (gate, up, down)]
    width, ff = gate.shape
    vmem = pl.BlockSpec(memory_space=pltpu.VMEM)
    return pl.pallas_call(
        lambda *refs: expert_body(count, *refs),
        in_specs=[vmem] * (count + 4),
        out_specs=[vmem, vmem],
        out_shape=[
            jax.ShapeDtypeStruct((all_rows // 2, width), jnp.bfloat16),
            jax.ShapeDtypeStruct((all_rows // 2, width), jnp.float32),
        ],
        scratch_shapes=[
            pltpu.VMEM((all_rows, wide), jnp.bfloat16),
            pltpu.VMEM((all_rows, ff), jnp.bfloat16),
        ],
        cost_estimate=pl.CostEstimate(
            flops=6 * all_rows * width * ff, transcendentals=all_rows * ff, bytes_accessed=2 * all_rows * width
        ),
        compiler_params=pltpu.CompilerParams(vmem_limit_bytes=24 << 20),
        name="expert",
    )(*blocks, place, gate, up, down)


def step(
    tokens, routes, gates, norm_gain, exp_gate, exp_up, exp_down, sh_gate, sh_up, sh_down, out_gain
):
    ep = lax.axis_size("ep")
    tp = lax.axis_size("tp")
    assert tp & (tp - 1) == 0 and ep & (ep - 1) == 0 and exp_gate.shape[0] == 1
    rows, width = tokens.shape
    half = width // tp
    chips = ep // 2
    me = lax.axis_index("ep")
    side = lax.axis_index("tp")
    f32, bf16 = jnp.float32, jnp.bfloat16

    def across(x, bits):
        return lax.ppermute(x, "ep", [(i, i ^ bits) for i in range(ep)])

    def over_tp(x, bits):
        return lax.ppermute(x, "tp", [(i, i ^ bits) for i in range(tp)])

    def features(x, index):
        if tp == 2:
            return jnp.where(index == 0, x[..., :half], x[..., half:])
        return lax.dynamic_slice_in_dim(x, index * half, half, axis=x.ndim - 1)

    values = tokens.astype(f32)
    normed = (
        values
        * lax.rsqrt(jnp.mean(values * values, axis=1, keepdims=True) + EPSILON)
        * norm_gain.astype(f32)
    ).astype(bf16)
    extra = (2 * ep + LANES - 1) // LANES * LANES
    column = jnp.arange(extra, dtype=jnp.int32)
    weight = jnp.sum(
        jnp.where(routes[:, :, None] == (column % ep)[None, None, :], gates[:, :, None], 0.0), axis=1
    )
    coarse = weight.astype(bf16)
    fine = (weight - coarse.astype(f32)).astype(bf16)
    packed = jnp.where(column < ep, coarse, jnp.where(column < 2 * ep, fine, jnp.zeros((), bf16)))
    block = jnp.concatenate([normed, packed], axis=1)

    place = ((column % ep == me) & (column < 2 * ep)).astype(f32)[None, :]
    chosen = (jnp.arange(width, dtype=jnp.int32) // half == side)[None, :]
    block, place, chosen = lax.optimization_barrier((block, place, chosen))

    mine = [block]
    for k in range(1, chips):
        mine.append(across(block, 2 * k))
    theirs = [across(b, 1) for b in mine]

    shared_gate = jnp.dot(normed, sh_gate, preferred_element_type=f32)
    shared_up = jnp.dot(normed, sh_up, preferred_element_type=f32)
    shared_hidden = (jax.nn.silu(shared_gate) * shared_up).astype(bf16)
    shared_part = jnp.dot(shared_hidden, sh_down, preferred_element_type=f32)

    weights = fetch(block[:16, :LANES], exp_gate, exp_up, exp_down)
    away, home = expert(theirs + mine, place, *weights)
    other = across(away, 1)
    paired = [
        home[k * rows : (k + 1) * rows] + other[k * rows : (k + 1) * rows].astype(f32)
        for k in range(chips)
    ]
    total = paired[0] + shared_part
    moved = [across(paired[k].astype(bf16), 2 * k) for k in range(1, chips)]
    for piece in moved:
        total = total + piece.astype(f32)
    sent = total.astype(bf16)
    for bits in range(1, tp):
        total = total + over_tp(sent, bits).astype(f32)
    scale = lax.rsqrt(jnp.mean(total * total, axis=1) + EPSILON)
    if tp == 2:
        total = jnp.where(chosen[:, :half], total[:, :half], total[:, half:])
    else:
        total = features(total, side)
    return (total * scale[:, None] * out_gain.astype(f32)).astype(bf16)


def solution(mesh):
    placed = (
        P(("grp", "ep"), None),
        P(("grp", "ep"), None),
        P(("grp", "ep"), None),
        P(),
        P("ep", None, "tp"),
        P("ep", None, "tp"),
        P("ep", "tp", None),
        P(None, "tp"),
        P(None, "tp"),
        P("tp", None),
        P("tp"),
    )
    return jax.shard_map(
        step, mesh=mesh, in_specs=placed, out_specs=P(("grp", "ep"), "tp"), check_vma=False
    )
```

```python
import jax
import jax.numpy as jnp
from jax import lax
from jax.experimental import pallas as pl
from jax.experimental.pallas import tpu as pltpu
from jax.sharding import PartitionSpec as P

EPSILON = 1e-06
LANES = 128


def prepare_body(ep, tokens, routes, gates, gain, out):
    width = tokens.shape[1]
    values = tokens[...].astype(jnp.float32)
    scale = lax.rsqrt(jnp.mean(values * values, axis=1, keepdims=True) + EPSILON)
    out[:, :width] = (values * scale * gain[...].astype(jnp.float32)).astype(jnp.bfloat16)
    shape = (tokens.shape[0], out.shape[1] - width)
    column = lax.broadcasted_iota(jnp.int32, shape, 1)
    name = jnp.where(column < ep, column, column - ep)
    weight = jnp.zeros(shape, jnp.float32)
    for k in range(routes.shape[1]):
        weight = weight + jnp.where(name == routes[:, k : k + 1], gates[:, k : k + 1], 0.0)
    coarse = weight.astype(jnp.bfloat16).astype(jnp.float32)
    packed = jnp.where(column < ep, coarse, jnp.where(column < 2 * ep, weight - coarse, 0.0))
    out[:, width:] = packed.astype(jnp.bfloat16)


def prepare(tokens, routes, gates, gain, ep, extra):
    rows, width = tokens.shape
    vmem = pl.BlockSpec(memory_space=pltpu.VMEM)
    return pl.pallas_call(
        lambda *refs: prepare_body(ep, *refs),
        in_specs=[vmem] * 4,
        out_specs=vmem,
        out_shape=jax.ShapeDtypeStruct((rows, width + extra), jnp.bfloat16),
        compiler_params=pltpu.CompilerParams(vmem_limit_bytes=8 << 20),
        name="prepare",
    )(tokens, routes, gates, gain[None, :])


def fetch_body(tie, gate, up, down, gate_out, up_out, down_out, sems):
    copies = [
        pltpu.make_async_copy(gate.at[0], gate_out, sems.at[0]),
        pltpu.make_async_copy(up.at[0], up_out, sems.at[1]),
        pltpu.make_async_copy(down.at[0], down_out, sems.at[2]),
    ]
    for copy in copies:
        copy.start()
    for copy in copies:
        copy.wait()


def fetch(tie, gate, up, down):
    hbm = pl.BlockSpec(memory_space=pltpu.HBM)
    gate, up, down = [pltpu.with_memory_space_constraint(w, pltpu.HBM) for w in (gate, up, down)]
    vmem = pl.BlockSpec(memory_space=pltpu.VMEM)
    return pl.pallas_call(
        fetch_body,
        in_specs=[vmem, hbm, hbm, hbm],
        out_specs=[vmem, vmem, vmem],
        out_shape=[pltpu.VMEM(w.shape[1:], w.dtype) for w in (gate, up, down)],
        scratch_shapes=[pltpu.SemaphoreType.DMA((3,))],
        cost_estimate=pl.CostEstimate(
            flops=4 * 10**9, transcendentals=0, bytes_accessed=2 * (gate.size + up.size + down.size)
        ),
        compiler_params=pltpu.CompilerParams(vmem_limit_bytes=2 << 20),
        name="fetch_weights",
    )(tie, gate, up, down)


def expert_body(count, *refs):
    blocks = refs[:count]
    place, gate, up, down, away, home, tokens, hidden = refs[count:]
    rows = blocks[0].shape[0]
    width = gate.shape[0]
    ff = gate.shape[1]
    step = min(256, ff)
    for i in range(count):
        tokens[i * rows : (i + 1) * rows, :] = blocks[i][...]
    lanes = tokens[:, width:].astype(jnp.float32)
    mix = jnp.sum(lanes * place[...], axis=1, keepdims=True)
    x = tokens[:, :width]
    for j in range(ff // step):
        cut = slice(j * step, (j + 1) * step)
        g = jnp.dot(x, gate[:, cut], preferred_element_type=jnp.float32)
        u = jnp.dot(x, up[:, cut], preferred_element_type=jnp.float32)
        hidden[:, cut] = (g / (1.0 + jnp.exp(-g)) * u * mix).astype(jnp.bfloat16)
    cutoff = away.shape[0]
    span = min(512, width)
    for j in range(width // span):
        cut = slice(j * span, (j + 1) * span)
        out = jnp.dot(hidden[...], down[:, cut], preferred_element_type=jnp.float32)
        away[:, cut] = out[:cutoff].astype(jnp.bfloat16)
        home[:, cut] = out[cutoff:]


def expert(blocks, place, gate, up, down):
    count = len(blocks)
    rows, wide = blocks[0].shape
    all_rows = count * rows
    gate, up, down = [pltpu.with_memory_space_constraint(w, pltpu.VMEM) for w in (gate, up, down)]
    width, ff = gate.shape
    vmem = pl.BlockSpec(memory_space=pltpu.VMEM)
    return pl.pallas_call(
        lambda *refs: expert_body(count, *refs),
        in_specs=[vmem] * (count + 4),
        out_specs=[vmem, vmem],
        out_shape=[
            jax.ShapeDtypeStruct((all_rows // 2, width), jnp.bfloat16),
            jax.ShapeDtypeStruct((all_rows // 2, width), jnp.float32),
        ],
        scratch_shapes=[
            pltpu.VMEM((all_rows, wide), jnp.bfloat16),
            pltpu.VMEM((all_rows, ff), jnp.bfloat16),
        ],
        cost_estimate=pl.CostEstimate(
            flops=6 * all_rows * width * ff, transcendentals=all_rows * ff, bytes_accessed=2 * all_rows * width
        ),
        compiler_params=pltpu.CompilerParams(vmem_limit_bytes=24 << 20),
        name="expert",
    )(*blocks, place, gate, up, down)


def step(
    tokens, routes, gates, norm_gain, exp_gate, exp_up, exp_down, sh_gate, sh_up, sh_down, out_gain
):
    ep = lax.axis_size("ep")
    tp = lax.axis_size("tp")
    assert tp & (tp - 1) == 0 and ep & (ep - 1) == 0 and exp_gate.shape[0] == 1
    rows, width = tokens.shape
    half = width // tp
    chips = ep // 2
    me = lax.axis_index("ep")
    side = lax.axis_index("tp")
    f32, bf16 = jnp.float32, jnp.bfloat16

    def across(x, bits):
        return lax.ppermute(x, "ep", [(i, i ^ bits) for i in range(ep)])

    def over_tp(x, bits):
        return lax.ppermute(x, "tp", [(i, i ^ bits) for i in range(tp)])

    def features(x, index):
        if tp == 2:
            return jnp.where(index == 0, x[..., :half], x[..., half:])
        return lax.dynamic_slice_in_dim(x, index * half, half, axis=x.ndim - 1)

    extra = (2 * ep + LANES - 1) // LANES * LANES
    column = jnp.arange(extra, dtype=jnp.int32)
    block = prepare(tokens, routes, gates, norm_gain, ep, extra)
    normed = block[:, :width]
    place = ((column % ep == me) & (column < 2 * ep)).astype(f32)[None, :]
    chosen = (jnp.arange(width, dtype=jnp.int32) // half == side)[None, :]
    block, place, chosen = lax.optimization_barrier((block, place, chosen))

    mine = [block]
    for k in range(1, chips):
        mine.append(across(block, 2 * k))
    theirs = [across(b, 1) for b in mine]

    shared_gate = jnp.dot(normed, sh_gate, preferred_element_type=f32)
    shared_up = jnp.dot(normed, sh_up, preferred_element_type=f32)
    shared_hidden = (jax.nn.silu(shared_gate) * shared_up).astype(bf16)
    shared_part = jnp.dot(shared_hidden, sh_down, preferred_element_type=f32)

    weights = fetch(block[:16, :LANES], exp_gate, exp_up, exp_down)
    away, home = expert(theirs + mine, place, *weights)
    other = across(away, 1)
    paired = [
        home[k * rows : (k + 1) * rows] + other[k * rows : (k + 1) * rows].astype(f32)
        for k in range(chips)
    ]
    total = paired[0] + shared_part
    moved = [across(paired[k].astype(bf16), 2 * k) for k in range(1, chips)]
    for piece in moved:
        total = total + piece.astype(f32)
    sent = total.astype(bf16)
    for bits in range(1, tp):
        total = total + over_tp(sent, bits).astype(f32)
    scale = lax.rsqrt(jnp.mean(total * total, axis=1) + EPSILON)
    if tp == 2:
        total = jnp.where(chosen[:, :half], total[:, :half], total[:, half:])
    else:
        total = features(total, side)
    return (total * scale[:, None] * out_gain.astype(f32)).astype(bf16)


def solution(mesh):
    placed = (
        P(("grp", "ep"), None),
        P(("grp", "ep"), None),
        P(("grp", "ep"), None),
        P(),
        P("ep", None, "tp"),
        P("ep", None, "tp"),
        P("ep", "tp", None),
        P(None, "tp"),
        P(None, "tp"),
        P("tp", None),
        P("tp"),
    )
    return jax.shard_map(
        step, mesh=mesh, in_specs=placed, out_specs=P(("grp", "ep"), "tp"), check_vma=False
    )
```
